32 devices in a mesh: sp: 16 (over z, y, x), tp: 2 (over core).
Axes of the slice: x: 2, y: 2, z: 4, core: 2. Of those that a mesh axis runs over, the one named last changes fastest.
Arguments:
- latent: bfloat16 [4096, 2048], P('sp'), may hold values from -6 to 6
- context: bfloat16 [512, 2048], P('sp'), may hold values from -6 to 6
- cond: bfloat16 [2048], P('sp'), may hold values from -6 to 6
- cond_ctx: bfloat16 [2048], P('sp'), may hold values from -6 to 6
- shift_weight: bfloat16 [2048, 2048], P('sp', 'tp'), may hold values from -0.125 to 0.125
- scale_weight: bfloat16 [2048, 2048], P('sp', 'tp'), may hold values from -0.125 to 0.125
- gate_weight: bfloat16 [2048, 2048], P('sp', 'tp'), may hold values from -0.25 to 0.25
- norm_gain: bfloat16 [2048], replicated, may hold values from 0.099609375 to 1.8984375
- query_weight: bfloat16 [2048, 1024], P(None, 'tp'), may hold values from -0.125 to 0.125
- key_weight: bfloat16 [2048, 1024], P(None, 'tp'), may hold values from -0.125 to 0.125
- value_weight: bfloat16 [2048, 1024], P(None, 'tp'), may hold values from -0.125 to 0.125
- query_gain: bfloat16 [64], replicated, may hold values from 0.099609375 to 1.8984375
- key_gain: bfloat16 [64], replicated, may hold values from 0.099609375 to 1.8984375
- offset_bias: float32 [16, 15, 31], P('tp'), may hold values from -0.5 to 251
- out_weight: bfloat16 [1024, 2048], P(None, 'tp'), may hold values from -1.5 to 1.5
Outputs:
- updated: bfloat16 [4096, 2048], P('sp', 'tp')
The draws below stay inside these ranges and needn't reach their ends.
All inputs are finite; a program needn't handle non-finite values.
Results may differ from the reference program's by a relative error of at most 0.0077.
Values may be sent and summed in bfloat16 or wider, within the bound.
No kernel may reach another device: no remote copies, remote signals or barrier semaphores. Data moves between devices by JAX's collectives and lax.ppermute only.
A program may use at most 128 MiB of HBM per device.

```python
import jax
import jax.numpy as jnp
from jax import lax

D = 2048
HEADS = 16
HEAD_DIM = 64
WIN_ROWS = 8
WIN_COLS = 16
GRID_W = 64
CTX = 512
TOKENS = 4096
HD = 1024


def draw_offset_bias(key, part):
    shape = (HEADS, 2 * WIN_ROWS - 1, 2 * WIN_COLS - 1)
    table = jax.random.uniform(jax.random.fold_in(key, 11), shape, jnp.float32, -0.5, 1.0)
    return table


def block_levels(rng, extent, cuts, low, largest):
    def one(position, shards_of):
        heights = jax.random.uniform(jax.random.fold_in(jax.random.fold_in(rng, 6), position), (shards_of,), jnp.float32, low / len(cuts), largest / len(cuts))
        return jnp.repeat(jnp.exp(heights), extent[position] // shards_of).reshape((-1,) + (1,) * (len(extent) - position - 1))

    factor_of = one(*cuts[0])
    for cut in cuts[1:]:
        factor_of = factor_of * one(*cut)
    return factor_of


def gaussian(key, dims, width, limit, shards=(), kind=jnp.bfloat16):
    level = block_levels(key, dims, shards, -0.22, 0.18) if shards else 1.0
    entries = jax.random.normal(key, dims, jnp.float32) * width * level
    return jnp.minimum(jnp.maximum(entries, -limit), limit).astype(kind)


def setup_inputs(seed: int = 0) -> dict:
    splits = jax.random.split(jax.random.key(seed), 16)
    latent = gaussian(splits[0], (TOKENS, D), 1.0, 6.0, ((0, 16),))
    context = gaussian(splits[1], (CTX, D), 1.0, 6.0, ((0, 16),))
    cond = gaussian(splits[2], (D,), 1.0, 6.0, ((0, 16),))
    cond_ctx = gaussian(splits[3], (D,), 1.0, 6.0, ((0, 16),))
    shift_weight = gaussian(splits[4], (D, D), D ** -0.5, 0.125, ((0, 16), (1, 2)))
    scale_weight = gaussian(splits[5], (D, D), D ** -0.5, 0.125, ((0, 16), (1, 2)))
    gate_weight = gaussian(splits[6], (D, D), (D // 4) ** -0.5, 0.25, ((0, 16), (1, 2)))
    norm_gain = jnp.clip(1.0 + 0.18 * jax.random.normal(splits[7], (D,), jnp.float32), 0.099609375, 1.8984375).astype(jnp.bfloat16)
    query_weight = gaussian(splits[8], (D, HD), D ** -0.5, 0.125, ((1, 2),))
    key_weight = gaussian(splits[9], (D, HD), D ** -0.5, 0.125, ((1, 2),))
    value_weight = gaussian(splits[10], (D, HD), D ** -0.5, 0.125, ((1, 2),))
    query_gain = jnp.clip(1.0 + 0.18 * jax.random.normal(splits[11], (HEAD_DIM,), jnp.float32), 0.099609375, 1.8984375).astype(jnp.bfloat16)
    key_gain = jnp.clip(1.0 + 0.18 * jax.random.normal(splits[12], (HEAD_DIM,), jnp.float32), 0.099609375, 1.8984375).astype(jnp.bfloat16)
    offset_bias = draw_offset_bias(jax.random.fold_in(splits[15], 71), 0)
    out_weight = gaussian(splits[14], (HD, D), (max(HD // 64, 1)) ** -0.5, 1.5, ((1, 2),))
    return {"latent": latent, "context": context, "cond": cond, "cond_ctx": cond_ctx, "shift_weight": shift_weight, "scale_weight": scale_weight, "gate_weight": gate_weight, "norm_gain": norm_gain, "query_weight": query_weight, "key_weight": key_weight, "value_weight": value_weight, "query_gain": query_gain, "key_gain": key_gain, "offset_bias": offset_bias, "out_weight": out_weight}


EPS = 1e-06

def modulate(rows, norm_gain, scale, shift):
    values = rows.astype(jnp.float32)
    normed = values * lax.rsqrt(lax.optimization_barrier(jnp.mean(values * values, axis=-1, keepdims=True)) + EPS)
    return (normed * norm_gain.astype(jnp.float32) * (1.0 + scale) + shift).astype(jnp.bfloat16)

def project_heads(hidden, weight, gain):
    raw = jnp.dot(hidden, weight, preferred_element_type=jnp.float32)
    split = raw.reshape(hidden.shape[0], -1, HEAD_DIM)
    if gain is None:
        return split.astype(jnp.bfloat16)
    normed = split * lax.rsqrt(lax.optimization_barrier(jnp.mean(split * split, axis=-1, keepdims=True)) + EPS)
    return (normed * gain.astype(jnp.float32)).astype(jnp.bfloat16)

def reference(latent, context, cond, cond_ctx, shift_weight, scale_weight, gate_weight, norm_gain, query_weight, key_weight, value_weight, query_gain, key_gain, offset_bias, out_weight):
    act = jax.nn.silu(cond.astype(jnp.float32)).astype(jnp.bfloat16)[None, :]
    act_ctx = jax.nn.silu(cond_ctx.astype(jnp.float32)).astype(jnp.bfloat16)[None, :]
    shift = jnp.dot(act, shift_weight, preferred_element_type=jnp.float32)[0]
    scale = jnp.dot(act, scale_weight, preferred_element_type=jnp.float32)[0]
    gate = jnp.dot(act, gate_weight, preferred_element_type=jnp.float32)[0]
    shift_ctx = jnp.dot(act_ctx, shift_weight, preferred_element_type=jnp.float32)[0]
    scale_ctx = jnp.dot(act_ctx, scale_weight, preferred_element_type=jnp.float32)[0]
    hidden = modulate(latent, norm_gain, scale, shift)
    queries = project_heads(hidden, query_weight, query_gain)
    keys = project_heads(hidden, key_weight, key_gain)
    values = project_heads(hidden, value_weight, None)
    hidden_ctx = modulate(context, norm_gain, scale_ctx, shift_ctx)
    ctx_keys = project_heads(hidden_ctx, key_weight, key_gain).astype(jnp.float32)
    ctx_values = project_heads(hidden_ctx, value_weight, None).astype(jnp.float32)
    total_rows = latent.shape[0] // GRID_W
    grid_q = queries.reshape(total_rows, GRID_W, HEADS, HEAD_DIM)
    grid_k = keys.reshape(total_rows, GRID_W, HEADS, HEAD_DIM)
    grid_v = values.reshape(total_rows, GRID_W, HEADS, HEAD_DIM)
    column = jnp.arange(GRID_W, dtype=jnp.int32)
    window_first = jnp.clip(column - WIN_COLS // 2, 0, GRID_W - WIN_COLS)
    inside = (column[None, :] >= window_first[:, None]) & (column[None, :] < window_first[:, None] + WIN_COLS)
    col_offset = jnp.clip(column[None, :] - column[:, None] + WIN_COLS - 1, 0, 2 * WIN_COLS - 2)
    by_col = offset_bias.astype(jnp.float32)[:, :, col_offset]
    factor = HEAD_DIM ** (-0.5)
    band_len = WIN_ROWS * GRID_W

    def one_row(row):
        first = jnp.clip(row - WIN_ROWS // 2, 0, total_rows - WIN_ROWS).astype(jnp.int32)
        band_k = lax.dynamic_slice_in_dim(grid_k, first, WIN_ROWS, 0).astype(jnp.float32)
        band_v = lax.dynamic_slice_in_dim(grid_v, first, WIN_ROWS, 0).astype(jnp.float32)
        query = lax.dynamic_index_in_dim(grid_q, row, 0, keepdims=False).astype(jnp.float32)
        row_offset = (first + jnp.arange(WIN_ROWS, dtype=jnp.int32) - row + WIN_ROWS - 1).astype(jnp.int32)
        bias = jnp.take(by_col, row_offset, axis=1)
        scores = jnp.einsum('qhd,jkhd->hqjk', query, band_k) * factor + jnp.transpose(bias, (0, 2, 1, 3))
        scores = jnp.where(inside[None, :, None, :], scores, -jnp.inf).reshape(HEADS, GRID_W, band_len)
        ctx_scores = jnp.einsum('qhd,chd->hqc', query, ctx_keys) * factor
        weights = jax.nn.softmax(jnp.concatenate([scores, ctx_scores], axis=-1), axis=-1).astype(jnp.bfloat16)
        weights = lax.optimization_barrier(weights).astype(jnp.float32)
        local_w = weights[..., :band_len].reshape(HEADS, GRID_W, WIN_ROWS, GRID_W)
        mixed = jnp.einsum('hqjk,jkhd->qhd', local_w, band_v) + jnp.einsum('hqc,chd->qhd', weights[..., band_len:], ctx_values)
        return mixed.astype(jnp.bfloat16).reshape(GRID_W, HEADS * HEAD_DIM)
    mixed = lax.map(one_row, jnp.arange(total_rows, dtype=jnp.int32)).reshape(latent.shape[0], HEADS * HEAD_DIM)
    projected = jnp.dot(mixed, out_weight, preferred_element_type=jnp.float32)
    return (latent.astype(jnp.float32) + gate[None, :] * projected).astype(jnp.bfloat16)
```

```python
import math

import jax
import jax.numpy as jnp
from jax import lax
from jax.experimental import pallas as pl
from jax.experimental.pallas import tpu as pltpu
from jax.sharding import PartitionSpec as P

HEAD_DIM = 64
WIN_ROWS = 8
WIN_COLS = 16
GRID_W = 64
REACH = WIN_ROWS // 2
LANES = 128
EPS = 1e-06
LOG2E = math.log2(math.e)
NEG = -1e30
F32 = jnp.float32
BF16 = jnp.bfloat16


def whole_spec(shape):
    return pl.BlockSpec(shape, lambda *_: (0,) * len(shape))


def smem_spec():
    return pl.BlockSpec(memory_space=pltpu.SMEM)


def partials_kernel(cond_ref, ctx_ref, shift_ref, scale_ref, gate_ref, out_ref):
    def act(ref):
        v = ref[...].astype(F32)
        return v / (1.0 + jnp.exp(-v))

    depth = cond_ref.shape[1]
    row = lax.broadcasted_iota(jnp.int32, (8, depth), 0)
    acts = jnp.where(row == 0, act(cond_ref), jnp.where(row == 1, act(ctx_ref), 0.0)).astype(BF16)
    shift = jnp.dot(acts, shift_ref[...], preferred_element_type=F32)
    scale = jnp.dot(acts, scale_ref[...], preferred_element_type=F32)
    gate = jnp.dot(acts, gate_ref[...], preferred_element_type=F32)
    out_ref[0:2, :] = shift[0:2]
    out_ref[2:4, :] = scale[0:2]
    out_ref[4:5, :] = gate[0:1]
    out_ref[5:8, :] = jnp.zeros((3, out_ref.shape[1]), F32)


def partials(cond, cond_ctx, shift_weight, scale_weight, gate_weight):
    return pl.pallas_call(
        partials_kernel,
        out_shape=jax.ShapeDtypeStruct((8, shift_weight.shape[1]), F32),
        name="partials",
    )(cond[None], cond_ctx[None], shift_weight, scale_weight, gate_weight)


def bias_kernel(rows, total, base_ref, table_ref, bias_ref, factor_ref, pair_ref):
    n_pairs = (rows + WIN_ROWS) // 2
    shape = (GRID_W, LANES)
    col = lax.broadcasted_iota(jnp.int32, shape, 0)
    lane = lax.broadcasted_iota(jnp.int32, shape, 1)
    left = jnp.clip(col - WIN_COLS // 2, 0, GRID_W - WIN_COLS)
    inside = (lane >= left) & (lane < left + WIN_COLS)
    low_half = lane < GRID_W
    n_off = 2 * WIN_ROWS - 1
    out = jnp.full(shape, NEG, F32)

    def tile(x):
        if not 0 <= x < n_off:
            return out
        line = jnp.broadcast_to(table_ref[0, x : x + 1, :], shape)
        rolled = pltpu.roll(line, LANES - (WIN_COLS - 1), 1, stride=1, stride_axis=0)
        return jnp.where(inside, rolled, NEG)

    tiles = {x: tile(x) for x in range(-1, n_off + 1)}
    for x in range(-1, n_off):
        pair_ref[x + 1] = jnp.where(low_half, tiles[x], pltpu.roll(tiles[x + 1], GRID_W, 1))
    base = base_ref[0]
    for r in range(rows):
        first = jnp.clip(base + r - REACH, 0, total - WIN_ROWS)
        masked = []
        top = jnp.zeros(shape, F32)
        for p in range(n_pairs):
            x = 2 * p - r + WIN_ROWS - 1 - REACH
            if x < -1 or x >= n_off:
                masked.append(None)
                continue
            kr = base + 2 * p - REACH
            ok = [jnp.where((kr + d >= first) & (kr + d < first + WIN_ROWS), 0.0, NEG) for d in (0, 1)]
            value = pair_ref[x + 1] + jnp.where(low_half, ok[0], ok[1])
            top = jnp.maximum(top, value)
            masked.append(value)
        peak = jnp.max(top, axis=-1, keepdims=True)
        q_rows = slice(r * GRID_W, (r + 1) * GRID_W)
        for p in range(n_pairs):
            value = out if masked[p] is None else (masked[p] - peak) * LOG2E
            bias_ref[0, q_rows, p * LANES : (p + 1) * LANES] = value
        factor_ref[0, q_rows, :] = jnp.broadcast_to(jnp.exp2(peak * -LOG2E), shape)


def bias_tables(offset_bias, rows, total, base):
    heads = offset_bias.shape[0]
    n_off = 2 * WIN_ROWS - 1
    table = jnp.pad(
        offset_bias,
        ((0, 0), (0, 0), (0, LANES - offset_bias.shape[2])),
        constant_values=NEG,
    )
    tokens = rows * GRID_W
    keys = (rows + WIN_ROWS) * GRID_W
    return pl.pallas_call(
        lambda *refs: bias_kernel(rows, total, *refs),
        grid=(heads,),
        in_specs=[smem_spec(), pl.BlockSpec((1, n_off, LANES), lambda h: (h, 0, 0))],
        out_specs=[
            pl.BlockSpec((1, tokens, keys), lambda h: (h, 0, 0)),
            pl.BlockSpec((1, tokens, LANES), lambda h: (h, 0, 0)),
        ],
        out_shape=[
            jax.ShapeDtypeStruct((heads, tokens, keys), F32),
            jax.ShapeDtypeStruct((heads, tokens, LANES), F32),
        ],
        scratch_shapes=[pltpu.VMEM((n_off + 1, GRID_W, LANES), F32)],
        name="bias_tables",
    )(base, table)


def project_kernel(row, normed, n_out, sel_ref, xa_ref, xb_ref, ma_ref, mb_ref, gain_ref, *refs):
    half = xa_ref.shape[1]
    weights = refs[:n_out]
    gains = refs[n_out : n_out + sum(normed)]
    outs = refs[n_out + sum(normed) : 2 * n_out + sum(normed)]
    hidden_ref = refs[-1]
    tokens = xa_ref.shape[0]
    step = min(tokens, 256)
    sel = sel_ref[0]
    spans = [
        pl.ds(pl.multiple_of(sel * half, LANES), half),
        pl.ds(pl.multiple_of((1 - sel) * half, LANES), half),
    ]
    lane = weights[0].shape[1]
    group = min(lane, 256)
    same = (
        lax.broadcasted_iota(jnp.int32, (group, group), 0) // HEAD_DIM
        == lax.broadcasted_iota(jnp.int32, (group, group), 1) // HEAD_DIM
    )
    ones = jnp.where(same, 1.0, 0.0).astype(BF16)
    for begin in range(0, tokens, step):
        rows = slice(begin, begin + step)
        parts = [ref[rows, :].astype(F32) for ref in (xa_ref, xb_ref)]
        total = sum(jnp.sum(p * p, axis=-1, keepdims=True) for p in parts)
        inv = lax.rsqrt(total * (1.0 / (2 * half)) + EPS)
        for part, span, mod in zip(parts, spans, (ma_ref, mb_ref)):
            gain = gain_ref[:, span] * (1.0 + mod[row + 2 : row + 3, :])
            hidden_ref[:, span] = (part * inv * gain + mod[row : row + 1, :]).astype(BF16)
        g = 0
        for weight, out, norm in zip(weights, outs, normed):
            raw = jnp.dot(hidden_ref[...], weight[...], preferred_element_type=F32)
            if not norm:
                out[rows, :] = raw.astype(BF16)
                continue
            squares = (raw * raw).astype(BF16)
            for c in range(0, lane, group):
                mean = jnp.dot(squares[:, c : c + group], ones, preferred_element_type=F32)
                scale = lax.rsqrt(mean * (1.0 / HEAD_DIM) + EPS) * gains[g][:, c : c + group]
                out[rows, c : c + group] = (raw[:, c : c + group] * scale).astype(BF16)
            g += 1


def project(name, row, sel, xa, xb, ma, mb, gain, weights, gains):
    normed = tuple(g is not None for g in gains)
    tokens, half = xa.shape
    lane = weights[0].shape[1]
    kept = [g for g in gains if g is not None]
    return pl.pallas_call(
        lambda *refs: project_kernel(row, normed, len(weights), *refs),
        in_specs=[smem_spec()] + [pl.BlockSpec(memory_space=pltpu.VMEM)] * (5 + len(weights) + len(kept)),
        out_shape=[jax.ShapeDtypeStruct((tokens, lane), BF16) for _ in weights],
        scratch_shapes=[pltpu.VMEM((min(tokens, 256), 2 * half), BF16)],
        name=name,
    )(sel, xa, xb, ma, mb, gain, *weights, *kept)


def attention_kernel(q_ref, ck_ref, cv_ref, k0, k1, k2, v0, v1, v2, bias_ref, factor_ref, out_ref):
    tokens, width = q_ref.shape
    n = width // HEAD_DIM
    lane = lax.broadcasted_iota(jnp.int32, (1, width), 1) // HEAD_DIM
    query = q_ref[...]
    sums = []
    for e in range(n):
        mine = query if n == 1 else jnp.where(lane == e, query, jnp.zeros_like(query))

        def values(ref):
            v = ref[...]
            if n == 1:
                return jnp.concatenate([v, jnp.ones_like(v)], axis=1)
            return jnp.where(lane == e, v, jnp.ones_like(v))

        def part(k_ref, v_ref, bias):
            score = lax.dot_general(
                mine, k_ref[...], (((1,), (1,)), ((), ())), preferred_element_type=F32
            )
            weight = jnp.exp2(score if bias is None else score + bias).astype(BF16)
            return jnp.dot(weight, values(v_ref), preferred_element_type=F32)

        total = part(ck_ref, cv_ref, None) * factor_ref[e]
        begin = 0
        for k_ref, v_ref in ((k0, v0), (k1, v1), (k2, v2)):
            count = k_ref.shape[0]
            total = total + part(k_ref, v_ref, bias_ref[e, :, begin : begin + count])
            begin += count
        sums.append(total)
    if n == 1:
        out_ref[...] = (sums[0][:, :HEAD_DIM] / sums[0][:, HEAD_DIM:]).astype(BF16)
        return
    num = jnp.where(lane == 0, sums[0], sums[1])
    den = pltpu.roll(jnp.where(lane == 0, sums[1], sums[0]), HEAD_DIM, 1)
    out_ref[...] = (num / den).astype(BF16)


def attention(q, ctx, keys, values, bias, factor):
    tokens, lane = q.shape
    width = min(lane, LANES)
    n = width // HEAD_DIM
    span = bias.shape[2]

    def cols(a):
        return pl.BlockSpec((a.shape[0], width), lambda h: (0, h))

    args = [q, *ctx, *keys, *values]
    return pl.pallas_call(
        attention_kernel,
        grid=(lane // width,),
        in_specs=[cols(a) for a in args]
        + [
            pl.BlockSpec((n, tokens, span), lambda h: (h, 0, 0)),
            pl.BlockSpec((n, tokens, LANES), lambda h: (h, 0, 0)),
        ],
        out_specs=cols(q),
        out_shape=jax.ShapeDtypeStruct((tokens, lane), BF16),
        name="attention",
    )(*args, bias, factor)


def output_kernel(sel_ref, parts_ref, mods_ref, latent_ref, weight_ref, out_ref):
    count, tokens, lane = parts_ref.shape
    total = jnp.zeros(out_ref.shape, F32)
    for p in range(count):
        which = jnp.where(sel_ref[0] == 0, p, count - 1 - p) if count == 2 else p
        rows = pl.ds(pl.multiple_of(which * lane, HEAD_DIM), lane)
        total += jnp.dot(parts_ref[p], weight_ref[rows, :], preferred_element_type=F32)
    out_ref[...] = (latent_ref[...].astype(F32) + mods_ref[4:5, :] * total).astype(BF16)


def output(sel, parts, mods, own, out_weight):
    return pl.pallas_call(
        output_kernel,
        in_specs=[smem_spec()] + [pl.BlockSpec(memory_space=pltpu.VMEM)] * 4,
        out_shape=jax.ShapeDtypeStruct(own.shape, BF16),
        name="output",
    )(sel, parts, mods, own, out_weight)


def stages(count):
    found, stride = [], 1
    while stride < count:
        radix = 4 if (count // stride) % 4 == 0 else count // stride
        found.append((stride, radix))
        stride *= radix
    return found


def peers(x, axis, stride, radix):
    count = lax.axis_size(axis)
    return [
        lax.ppermute(x, axis, [(i, i ^ (k * stride)) for i in range(count)]) for k in range(1, radix)
    ]


def body(
    latent, context, cond, cond_ctx, shift_weight, scale_weight, gate_weight, norm_gain,
    query_weight, key_weight, value_weight, query_gain, key_gain, offset_bias, out_weight,
):
    sp, tp = lax.axis_size("sp"), lax.axis_size("tp")
    at_sp, at_tp = lax.axis_index("sp"), lax.axis_index("tp")
    width = latent.shape[1]
    share = width // tp
    half = width // 2
    heads = offset_bias.shape[0]
    rows = latent.shape[0] // GRID_W
    total = rows * sp
    edge = REACH * GRID_W
    sel = (at_tp if tp == 2 else at_tp * 0).astype(jnp.int32)[None]
    base = (at_sp * rows).astype(jnp.int32)[None]

    def halves(mine):
        if tp == 2:
            return mine, lax.ppermute(mine, "tp", [(0, 1), (1, 0)])
        full = lax.all_gather(mine, "tp", axis=1, tiled=True)
        return full[:, :half], full[:, half:]

    own = lax.dynamic_slice_in_dim(latent, at_tp * share, share, 1)
    ctx = lax.dynamic_slice_in_dim(context, at_tp * share, share, 1)

    mods = partials(cond, cond_ctx, shift_weight, scale_weight, gate_weight)
    for stride, radix in stages(sp):
        mods = mods + sum(peers(mods, "sp", stride, radix))
    ma, mb = halves(mods)

    line = [(i, i + 1) for i in range(sp - 1)]
    low = lax.ppermute(own[-edge:], "sp", line)
    high = lax.ppermute(own[:edge], "sp", [(b, a) for a, b in line])
    for stride, radix in stages(sp)[::-1]:
        ctx = jnp.concatenate([ctx, *peers(ctx, "sp", stride, radix)], axis=0)
    ca, cb = halves(ctx)
    la, lb = halves(low)
    ha, hb = halves(high)

    bias, factor = bias_tables(offset_bias, rows, total, base)
    gain = norm_gain.astype(F32)[None]
    q_gain = jnp.tile(query_gain.astype(F32) * (HEAD_DIM**-0.5 * LOG2E), heads)[None]
    k_gain = jnp.tile(key_gain.astype(F32), heads)[None]
    kv = ([key_weight, value_weight], [k_gain, None])
    ck, cv = project("ctx_kv", 1, sel, ca, cb, ma, mb, gain, *kv)
    if tp == 2:
        other = lax.dynamic_slice_in_dim(latent, (1 - at_tp) * share, share, 1)
        xa, xb = own, other
    else:
        xa, xb = latent[:, :half], latent[:, half:]
    q, k1, v1 = project(
        "own_qkv", 0, sel, xa, xb, ma, mb, gain,
        [query_weight, key_weight, value_weight], [q_gain, k_gain, None],
    )
    k0, v0 = project("low_kv", 0, sel, la, lb, ma, mb, gain, *kv)
    k2, v2 = project("high_kv", 0, sel, ha, hb, ma, mb, gain, *kv)
    mixed = attention(q, (ck, cv), (k0, k1, k2), (v0, v1, v2), bias, factor)
    if tp == 2:
        parts = jnp.stack([mixed, lax.ppermute(mixed, "tp", [(0, 1), (1, 0)])])
    else:
        parts = lax.all_gather(mixed, "tp", axis=1, tiled=True)[None]
    return output(sel, parts, mods, own, out_weight)


def solution(mesh):
    in_specs = (
        P("sp", None),
        P("sp", None),
        P("sp"),
        P("sp"),
        P("sp", "tp"),
        P("sp", "tp"),
        P("sp", "tp"),
        P(),
        P(None, "tp"),
        P(None, "tp"),
        P(None, "tp"),
        P(),
        P(),
        P("tp", None, None),
        P(None, "tp"),
    )
    out_specs = P("sp", "tp")
    return jax.shard_map(body, mesh=mesh, in_specs=in_specs, out_specs=out_specs, check_vma=False)
```
